32 devices in a mesh: sp: 8 (over z, x), tp: 4 (over y, core).
Axes of the slice: x: 2, y: 2, z: 4, core: 2. Of those that a mesh axis runs over, the one named last changes fastest.
Arguments:
- residual: bfloat16 [4096, 2048], P('sp'), may hold values from -80 to 80
- queries: bfloat16 [4096, 1024], P('sp', 'tp'), may hold values from -260 to 260
- keys: bfloat16 [4096, 512], P('sp', 'tp'), may hold values from -7 to 7
- values: bfloat16 [4096, 512], P('sp', 'tp'), may hold values from -12 to 12
- documents: int32 [4096], P('sp'), may hold values from 0 to 3, never falling along the last dimension, each value on 1 to 3072 neighbouring positions
- sinks: float32 [16], P('tp'), may hold values from 1 to 6
- out_weight: bfloat16 [1024, 2048], P('tp'), may hold values from -0.5 to 0.5
- norm_gain: float32 [2048], replicated, may hold values from 0.1 to 1.9
- gate_weight: bfloat16 [2048, 5632], P('sp', 'tp'), may hold values from -0.125 to 0.125
- up_weight: bfloat16 [2048, 5632], P('sp', 'tp'), may hold values from -0.125 to 0.125
- down_weight: bfloat16 [2048, 5632], P('sp', 'tp'), may hold values from -0.078125 to 0.078125
Outputs:
- mixed: bfloat16 [4096, 2048], P('sp', 'tp')
The draws below stay inside these ranges and needn't reach their ends.
Inputs may be any that keep to these rules, and one draw needn't show every extreme that they name: `documents`: document numbers never fall along the positions; a document holds at most 3072 positions.
All inputs are finite; a program needn't handle non-finite values.
Results may differ from the reference program's by a relative error of at most 0.01.
Values may be sent and summed in bfloat16 or wider, within the bound.
A program may use at most 64 MiB of HBM per device.

```python
import math
import jax
import jax.numpy as jnp
import numpy as np
from jax import lax

D = 2048
HEADS = 16
KV_HEADS = 8
HEAD_DIM = 64
FF = 5632
WINDOW = 128
GROUP = 2
D_ATT = 1024
TOKENS = 4096
DOC_MOST = 3072
N_SP = 8
N_TP = 4


def drawn_keys(key):
    return jnp.clip(jax.random.normal(jax.random.fold_in(key, 11), (TOKENS, KV_HEADS * HEAD_DIM), jnp.float32), -6.0, 6.0)


def draw_keys(key, part):
    base_keys = drawn_keys(key)
    return base_keys.astype(jnp.bfloat16)


def draw_queries(key, part):
    entries = jnp.clip(jax.random.normal(jax.random.fold_in(key, 21), (TOKENS, HEADS * HEAD_DIM), jnp.float32), -6.0, 6.0)
    return entries.astype(jnp.bfloat16)


def draw_residual(key, part):
    col_scale = jnp.exp(jnp.linspace(jnp.log(0.5), jnp.log(3.0), D, dtype=jnp.float32))[None, :]
    row_scale = jnp.exp(jax.random.uniform(jax.random.fold_in(key, 31), (TOKENS, 1), jnp.float32, jnp.log(0.5), jnp.log(3.0)))
    entries = jnp.clip(jax.random.normal(jax.random.fold_in(key, 32), (TOKENS, D), jnp.float32), -6.0, 6.0)
    return (entries * row_scale * col_scale).astype(jnp.bfloat16)


def steps_of(key, extent, shards, least, top_value):
    def one(axis_at, parts):
        draws = jax.random.uniform(jax.random.fold_in(jax.random.fold_in(key, 6), axis_at), (parts,), jnp.float32, least / len(shards), top_value / len(shards))
        return jnp.repeat(jnp.exp(draws), extent[axis_at] // parts).reshape((-1,) + (1,) * (len(extent) - axis_at - 1))

    factor_of = one(*shards[0])
    for cut in shards[1:]:
        factor_of = factor_of * one(*cut)
    return factor_of


def length_profile(count, total, most, skew):
    loads = [(1 << 20) // math.isqrt(standing ** skew) + 1 for standing in range(2, count + 1)]
    rest, counts = total - most - (count - 1), [1] * (count - 1)
    while rest > 0:
        movable = [i for i in range(count - 1) if counts[i] < most]
        pool, remaining = sum([loads[i] for i in movable]), rest
        for i in movable:
            more = min(most - counts[i], max(1, remaining * loads[i] // pool), rest)
            counts[i] = counts[i] + more
            rest = rest - more
    return np.array([most] + counts)


def uneven_parts(key, count, total, reach, slope):
    if count == 2:
        one = jax.random.randint(key, (), max(1, total - reach), min(reach, total - 1) + 1)
        return jnp.stack([one, total - one])
    tallies = jnp.asarray(length_profile(count, total, reach, slope), jnp.int32)
    twos = (count - 1) // 2
    donor, sink = tallies[1:1 + 2 * twos:2], tallies[2:2 + 2 * twos:2]
    room = jnp.minimum(donor - 1, reach - sink)
    moved = jax.random.randint(jax.random.fold_in(key, 1), (twos,), 0, 1 << 20) % (room + 1)
    tallies = tallies.at[1:1 + 2 * twos:2].set(donor - moved).at[2:2 + 2 * twos:2].set(sink + moved)
    return tallies[jax.random.permutation(jax.random.fold_in(key, 2), count)]


def centred(key, shape, width, reach, split=(), kind=jnp.bfloat16):
    drawn = jax.random.normal(key, shape, jnp.float32) * width
    if len(split) > 0:
        drawn = steps_of(key, shape, split, -0.22, 0.18) * drawn
    return jnp.clip(drawn, min=-reach, max=reach).astype(kind)


def setup_inputs(seed: int = 0) -> dict:
    seeds = jax.random.split(jax.random.key(seed), 12)
    return {
        "residual": draw_residual(jax.random.fold_in(seeds[11], 71), 0),
        "queries": draw_queries(jax.random.fold_in(seeds[11], 71), 0),
        "keys": draw_keys(jax.random.fold_in(seeds[11], 71), 0),
        "values": centred(seeds[3], (TOKENS, KV_HEADS * HEAD_DIM), 2.0, 12.0, ((0, 8), (1, 4))),
        "documents": jnp.searchsorted(jnp.cumsum(uneven_parts(seeds[4], N_SP // 2, TOKENS, DOC_MOST, 1)), jnp.arange(TOKENS), side="right").astype(jnp.int32),
        "sinks": jnp.clip(1.0 + 5.0 * jax.random.uniform(seeds[5], (HEADS,), jnp.float32) ** steps_of(seeds[5], (HEADS,), ((0, 4),), -0.2, 0.2), 1.0, 6.0),
        "out_weight": centred(seeds[6], (D_ATT, D), (2 * HEAD_DIM) ** -0.5, 0.5, ((0, 4),)),
        "norm_gain": jnp.clip(1.0 + 0.18 * jax.random.normal(seeds[7], (D,), jnp.float32), 0.1, 1.9),
        "gate_weight": centred(seeds[8], (D, FF), D ** -0.5, 0.125, ((0, 8), (1, 4))),
        "up_weight": centred(seeds[9], (D, FF), D ** -0.5, 0.125, ((0, 8), (1, 4))),
        "down_weight": centred(seeds[10], (D, FF), FF ** -0.5, 0.078125, ((0, 8), (1, 4))),
    }


neg_big = -1e+30
norm_eps = 1e-05

def attend(queries, keys, values, documents, sinks):
    total_rows = queries.shape[0]
    block_count = total_rows // WINDOW
    q_blocks = queries.astype(jnp.float32).reshape(block_count, WINDOW, KV_HEADS, GROUP, HEAD_DIM)
    k_blocks = keys.astype(jnp.float32).reshape(block_count, WINDOW, KV_HEADS, HEAD_DIM)
    v_blocks = values.astype(jnp.float32).reshape(block_count, WINDOW, KV_HEADS, HEAD_DIM)
    zero_block = jnp.zeros_like(k_blocks[:1])
    k_band = jnp.concatenate([jnp.concatenate([zero_block, k_blocks[:-1]], axis=0), k_blocks], axis=1)
    v_band = jnp.concatenate([jnp.concatenate([zero_block, v_blocks[:-1]], axis=0), v_blocks], axis=1)
    doc_own = documents.astype(jnp.int32).reshape(block_count, WINDOW)
    doc_prev = jnp.concatenate([jnp.zeros((1, WINDOW), jnp.int32), doc_own[:-1]], axis=0)
    doc_band = jnp.concatenate([doc_prev, doc_own], axis=1)
    row_idx = jnp.arange(WINDOW, dtype=jnp.int32)
    col_idx = jnp.arange(2 * WINDOW, dtype=jnp.int32)
    first = jnp.arange(block_count, dtype=jnp.int32) * WINDOW
    q_pos = first[:, None] + row_idx[None, :]
    k_pos = first[:, None] - WINDOW + col_idx[None, :]
    distance = q_pos[:, :, None] - k_pos[:, None, :]
    visible = (distance >= 0) & (distance < WINDOW) & (k_pos[:, None, :] >= 0) & (doc_own[:, :, None] == doc_band[:, None, :])
    scores = jnp.einsum('nikgd,njkd->nkgij', q_blocks, k_band) * HEAD_DIM ** (-0.5)
    scores = jnp.where(visible[:, None, None], scores, neg_big)
    sink_logit = sinks.astype(jnp.float32).reshape(1, KV_HEADS, GROUP, 1, 1)
    row_max = jnp.maximum(scores.max(-1, keepdims=True), sink_logit)
    expo = jnp.where(visible[:, None, None], jnp.exp(scores - row_max), 0.0)
    denom_sum = expo.sum(-1, keepdims=True) + jnp.exp(sink_logit - row_max)
    weights = (expo / denom_sum).astype(jnp.bfloat16)
    mixed = jnp.einsum('nkgij,njkd->nikgd', weights.astype(jnp.float32), v_band)
    return mixed.reshape(total_rows, D_ATT).astype(jnp.bfloat16)

def reference(residual, queries, keys, values, documents, sinks, out_weight, norm_gain, gate_weight, up_weight, down_weight):
    attended = attend(queries, keys, values, documents, sinks)
    head_cols = D_ATT // N_TP
    projected = jnp.zeros((TOKENS, D), jnp.float32)
    for index_tp in range(N_TP):
        partial_sum = jnp.dot(attended[:, index_tp * head_cols:(index_tp + 1) * head_cols], out_weight[index_tp * head_cols:(index_tp + 1) * head_cols], preferred_element_type=jnp.float32)
        projected = projected + lax.optimization_barrier(partial_sum.astype(jnp.bfloat16)).astype(jnp.float32)
    after = (residual.astype(jnp.float32) + projected).astype(jnp.bfloat16)
    after_f = after.astype(jnp.float32)
    inv_rms = lax.rsqrt(lax.optimization_barrier(jnp.mean(after_f * after_f, axis=1, keepdims=True)) + norm_eps)
    normed = (after_f * inv_rms * norm_gain[None, :]).astype(jnp.bfloat16)
    gate_act = jnp.dot(normed, gate_weight, preferred_element_type=jnp.float32)
    up_act = jnp.dot(normed, up_weight, preferred_element_type=jnp.float32)
    hidden = (jax.nn.silu(gate_act) * up_act).astype(jnp.bfloat16)
    unit_cols = FF // N_TP
    down_sum = jnp.zeros((TOKENS, D), jnp.float32)
    for index_tp in range(N_TP):
        partial_sum = lax.dot_general(hidden[:, index_tp * unit_cols:(index_tp + 1) * unit_cols], down_weight[:, index_tp * unit_cols:(index_tp + 1) * unit_cols], (((1,), (1,)), ((), ())), preferred_element_type=jnp.float32)
        down_sum = down_sum + lax.optimization_barrier(partial_sum.astype(jnp.bfloat16)).astype(jnp.float32)
    return (after.astype(jnp.float32) + down_sum).astype(jnp.bfloat16)
```

```python
import functools

import jax
import jax.numpy as jnp
from jax import lax
from jax.experimental import pallas as pl
from jax.experimental.pallas import tpu as pltpu
from jax.sharding import PartitionSpec as P

HEAD_DIM = 64
WINDOW = 128
GROUP = 2


neg_big = -1e30
norm_eps = 1e-05


def from_behind(shard, axis, by):
    length = lax.axis_size(axis)
    pairs = [(i, i + by) for i in range(length) if 0 <= i + by < length]
    return lax.ppermute(shard, axis, pairs)


def attend(queries, keys, values, documents, sinks, tail_keys, tail_values, tail_docs, offset):
    rows_here = queries.shape[0]
    block_count = rows_here // WINDOW
    kv_here = keys.shape[1] // HEAD_DIM
    q_blocks = queries.reshape(block_count, WINDOW, kv_here, GROUP, HEAD_DIM)
    k_blocks = keys.reshape(block_count, WINDOW, kv_here, HEAD_DIM)
    v_blocks = values.reshape(block_count, WINDOW, kv_here, HEAD_DIM)
    k_prev = jnp.concatenate(
        [tail_keys.reshape(1, WINDOW, kv_here, HEAD_DIM), k_blocks[:-1]], axis=0
    )
    v_prev = jnp.concatenate(
        [tail_values.reshape(1, WINDOW, kv_here, HEAD_DIM), v_blocks[:-1]], axis=0
    )
    k_band = jnp.concatenate([k_prev, k_blocks], axis=1)
    v_band = jnp.concatenate([v_prev, v_blocks], axis=1)
    doc_own = documents.astype(jnp.float32).reshape(block_count, WINDOW)
    doc_prev = jnp.concatenate(
        [tail_docs.astype(jnp.float32).reshape(1, WINDOW), doc_own[:-1]], axis=0
    )
    doc_band = jnp.concatenate([doc_prev, doc_own], axis=1)
    row_idx = jnp.arange(WINDOW, dtype=jnp.int32)
    col_idx = jnp.arange(2 * WINDOW, dtype=jnp.int32)
    first = offset + jnp.arange(block_count, dtype=jnp.int32) * WINDOW
    q_pos = first[:, None] + row_idx[None, :]
    k_pos = first[:, None] - WINDOW + col_idx[None, :]
    distance = q_pos[:, :, None] - k_pos[:, None, :]
    visible = (
        (distance >= 0)
        & (distance < WINDOW)
        & (k_pos[:, None, :] >= 0)
        & (doc_own[:, :, None] == doc_band[:, None, :])
    )
    scores = jnp.einsum(
        "nikgd,njkd->nkgij", q_blocks, k_band, preferred_element_type=jnp.float32
    ) * HEAD_DIM ** (-0.5)
    scores = jnp.where(visible[:, None, None], scores, neg_big)
    sink_logit = sinks.reshape(1, kv_here, GROUP, 1, 1)
    row_max = jnp.maximum(scores.max(-1, keepdims=True), sink_logit)
    expo = jnp.where(visible[:, None, None], jnp.exp(scores - row_max), 0.0)
    denom_sum = expo.sum(-1, keepdims=True) + jnp.exp(sink_logit - row_max)
    weights = (expo / denom_sum).astype(jnp.bfloat16)
    mixed = jnp.einsum("nkgij,njkd->nikgd", weights, v_band, preferred_element_type=jnp.float32)
    return mixed.reshape(rows_here, kv_here * GROUP * HEAD_DIM).astype(jnp.bfloat16)


def on_device(
    residual,
    queries,
    keys,
    values,
    documents,
    sinks,
    out_weight,
    norm_gain,
    gate_weight,
    up_weight,
    down_weight,
):
    rows_here = queries.shape[0]
    offset = lax.axis_index("sp") * rows_here
    doc_tail = documents[rows_here - WINDOW :].astype(jnp.bfloat16)
    tail_keys, tail_values, tail_docs = from_behind(
        (keys[rows_here - WINDOW :], values[rows_here - WINDOW :], doc_tail), "sp", 1
    )
    attended = attend(
        queries, keys, values, documents, sinks, tail_keys, tail_values, tail_docs, offset
    )
    model_width = residual.shape[1]
    col_count = model_width // lax.axis_size("tp")
    col_first = lax.axis_index("tp") * col_count
    full_term = jnp.dot(attended, out_weight, preferred_element_type=jnp.float32)
    projected = lax.psum(full_term.astype(jnp.bfloat16), "tp").astype(jnp.float32)
    after_full = (residual.astype(jnp.float32) + projected).astype(jnp.bfloat16)
    after_f = after_full.astype(jnp.float32)
    inv_rms = lax.rsqrt(jnp.mean(after_f * after_f, axis=1, keepdims=True) + norm_eps)
    normed = (after_f * inv_rms * norm_gain[None, :]).astype(jnp.bfloat16)
    after = lax.dynamic_slice_in_dim(after_full, col_first, col_count, 1)
    gate_act = jnp.dot(
        normed,
        lax.all_gather(gate_weight, "sp", axis=0, tiled=True),
        preferred_element_type=jnp.float32,
    )
    up_act = jnp.dot(
        normed,
        lax.all_gather(up_weight, "sp", axis=0, tiled=True),
        preferred_element_type=jnp.float32,
    )
    down_full = lax.all_gather(down_weight, "sp", axis=0, tiled=True)
    hidden = (jax.nn.silu(gate_act) * up_act).astype(jnp.bfloat16)
    summed = lax.psum_scatter(
        lax.dot_general(
            down_full, hidden, (((1,), (1,)), ((), ())), preferred_element_type=jnp.float32
        ).astype(jnp.bfloat16),
        "tp",
        scatter_dimension=0,
        tiled=True,
    ).astype(jnp.float32)
    return (after.astype(jnp.float32) + summed.T).astype(jnp.bfloat16)


MESH = pl.DeviceIdType.MESH
NT = (((1,), (1,)), ((), ()))


def dot(a, b, dims=(((1,), (0,)), ((), ()))):
    return lax.dot_general(a, b, dims, preferred_element_type=jnp.float32)


def kernel(
    S, T,
    res_hbm, q_ref, k_ref, v_ref, doc_ref, sink_ref, ow_hbm, gain_ref, g_hbm, u_hbm, d_hbm,
    out_ref,
    G, kx, vx, dx, att, res_v, ow_v, psend, precv, after, normed, ga, ua, hidden, dsend, drecv,
    w_send, w_recv, tail_send, tail_recv, loc, p_send, p_recv, a_send, a_recv, d_send, d_recv,
):
    s = lax.axis_index("sp")
    t = lax.axis_index("tp")
    R = q_ref.shape[0]
    D = gain_ref.shape[1]
    C = D // T
    K = D // S
    F = g_hbm.shape[1]
    HK = K // 2
    PER = C // K
    z, x = s // 2, s % 2
    zp = ((z + 1) % 4) * 2 + x
    zm = ((z + 3) % 4) * 2 + x
    z2 = ((z + 2) % 4) * 2 + x
    xp = z * 2 + (1 - x)
    zp_x = ((z + 1) % 4) * 2 + (1 - x)
    zm_x = ((z + 3) % 4) * 2 + (1 - x)
    z2_x = ((z + 2) % 4) * 2 + (1 - x)
    after_s = (s + 1) % S
    before_s = (s + S - 1) % S

    weights = (g_hbm, u_hbm, d_hbm)
    local = [
        pltpu.make_async_copy(weights[m], G.at[m, s], loc.at[m]) for m in range(3)
    ]
    local.append(pltpu.make_async_copy(ow_hbm, ow_v, loc.at[3]))
    local.append(pltpu.make_async_copy(
        res_hbm.at[:, pl.ds(pl.multiple_of(t * C, C), C)], res_v, loc.at[4]))
    for c in (local[3], local[4], local[0], local[1], local[2]):
        c.start()

    barrier = pltpu.get_barrier_semaphore()
    peers = [(zp, t), (zm, t), (xp, t), (after_s, t), (before_s, t)]
    peers += [(s, (t + d) % T) for d in range(1, T)]
    for p in peers:
        pl.semaphore_signal(barrier, inc=1, device_id=p, device_id_type=MESH)
    pl.semaphore_wait(barrier, len(peers))

    started = []

    tails = []
    for i, (a, b) in enumerate((
        (k_ref.at[pl.ds(R - WINDOW, WINDOW)], kx.at[pl.ds(0, WINDOW)]),
        (v_ref.at[pl.ds(R - WINDOW, WINDOW)], vx.at[pl.ds(0, WINDOW)]),
        (doc_ref.at[pl.ds(doc_ref.shape[0] - 8, 8)], dx.at[pl.ds(0, 8)]),
    )):
        c = pltpu.make_async_remote_copy(
            src_ref=a, dst_ref=b, send_sem=tail_send.at[i], recv_sem=tail_recv.at[i],
            device_id=(after_s, t), device_id_type=MESH)
        c.start()
        tails.append(c)

    target = (zp, zm, xp)
    count = [0, 0, 0]

    def send(link, m, src, h, own=False):
        part = pl.ds(h * HK, HK)
        place = G.at[m, src, part]
        c = pltpu.make_async_remote_copy(
            src_ref=weights[m].at[part] if own else place, dst_ref=place,
            send_sem=w_send.at[link, count[link]], recv_sem=w_recv.at[m, src, h],
            device_id=(target[link], t), device_id_type=MESH)
        count[link] += 1
        c.start()
        started.append(c)

    def recv(m, src, h):
        place = G.at[m, src, pl.ds(h * HK, HK)]
        pltpu.make_async_remote_copy(
            src_ref=place, dst_ref=place, send_sem=w_send.at[0, 0],
            recv_sem=w_recv.at[m, src, h], device_id=(zp, t), device_id_type=MESH).wait_recv()

    for m in (0, 1):
        for h in (0, 1):
            for link in (0, 1, 2):
                send(link, m, s, h, own=True)

    kx[pl.ds(WINDOW, R), :] = k_ref[...]
    vx[pl.ds(WINDOW, R), :] = v_ref[...]
    dx[pl.ds(8, doc_ref.shape[0]), :] = doc_ref[...]
    for c in tails:
        c.wait_recv()
    heads = q_ref.shape[1] // HEAD_DIM

    def block(b, carry):
        rows = pl.ds(pl.multiple_of(b * WINDOW, WINDOW), WINDOW)
        band = pl.ds(pl.multiple_of(b * WINDOW, WINDOW), 2 * WINDOW)
        prev = dx[pl.ds(pl.multiple_of(b * 8, 8), 8), :][0:1].astype(jnp.float32)
        own = dx[pl.ds(pl.multiple_of(b * 8 + 8, 8), 8), :][0:1].astype(jnp.float32)
        doc_q = jnp.broadcast_to(own, (WINDOW, WINDOW)).T
        i = lax.broadcasted_iota(jnp.int32, (WINDOW, WINDOW), 0)
        j = lax.broadcasted_iota(jnp.int32, (WINDOW, WINDOW), 1)
        first = s * R + b * WINDOW - WINDOW
        see_prev = (j > i) & (doc_q == prev) & (first + j >= 0)
        see_own = (j <= i) & (doc_q == own)
        visible = jnp.concatenate(
            [see_prev.astype(jnp.float32), see_own.astype(jnp.float32)], axis=1) > 0.5
        for h in range(heads):
            kv = h // GROUP
            cols = slice(kv * HEAD_DIM, (kv + 1) * HEAD_DIM)
            q = q_ref[rows, h * HEAD_DIM:(h + 1) * HEAD_DIM]
            scores = dot(q, kx[band, cols], NT) * HEAD_DIM ** (-0.5)
            scores = jnp.where(visible, scores, neg_big)
            sink = sink_ref[h]
            row_max = jnp.maximum(scores.max(-1, keepdims=True), sink)
            expo = jnp.where(visible, jnp.exp(scores - row_max), 0.0)
            total = expo.sum(-1, keepdims=True) + jnp.exp(sink - row_max)
            w = (expo / total).astype(jnp.bfloat16)
            att[rows, h * HEAD_DIM:(h + 1) * HEAD_DIM] = dot(w, vx[band, cols]).astype(jnp.bfloat16)
        return carry

    lax.fori_loop(0, R // WINDOW, block, 0)

    local[3].wait()
    reach = [(t + d) % T for d in (2, 1, 3)]
    psent = []
    for n, owner in enumerate(reach + [t]):
        cols = pl.ds(pl.multiple_of(owner * C, C), C)
        value = dot(att[...], ow_v[:, cols]).astype(jnp.bfloat16)
        if n == T - 1:
            precv[t] = value
        else:
            psend[owner] = value
            c = pltpu.make_async_remote_copy(
                src_ref=psend.at[owner], dst_ref=precv.at[t], send_sem=p_send.at[n],
                recv_sem=p_recv.at[t], device_id=(s, owner), device_id_type=MESH)
            c.start()
            psent.append(c)

    def recv_block(buf, sems, source):
        pltpu.make_async_remote_copy(
            src_ref=buf.at[source], dst_ref=buf.at[source], send_sem=p_send.at[0],
            recv_sem=sems.at[source], device_id=(s, (t + 1) % T), device_id_type=MESH).wait_recv()

    recv(0, zm, 0)
    send(0, 0, zm, 0)
    recv(0, zp, 1)
    send(1, 0, zp, 1)
    recv(0, zm, 1)
    recv(0, zp, 0)
    send(2, 0, zm, 1)
    send(2, 0, zp, 1)
    recv(1, zm, 0)
    send(0, 1, zm, 0)
    recv(1, zp, 1)
    send(1, 1, zp, 1)
    recv(1, zm, 1)
    recv(1, zp, 0)
    recv(0, xp, 0)
    recv(0, xp, 1)
    recv(1, xp, 0)
    recv(1, xp, 1)
    for m, h in ((0, 0), (1, 0), (1, 1)):
        send(0, m, xp, h)
        send(1, m, xp, h)
    send(0, 2, s, 0, own=True)
    send(0, 2, s, 1, own=True)
    send(1, 2, s, 1, own=True)
    send(1, 2, s, 0, own=True)

    local[4].wait()
    for owner in reach:
        recv_block(precv, p_recv, owner)
    total = precv[0].astype(jnp.float32)
    for i in range(1, T):
        total += precv[i].astype(jnp.float32)
    after[t] = (res_v[...].astype(jnp.float32) + total).astype(jnp.bfloat16)
    asent = []
    for n, peer in enumerate(reach):
        c = pltpu.make_async_remote_copy(
            src_ref=after.at[t], dst_ref=after.at[t], send_sem=a_send.at[n],
            recv_sem=a_recv.at[t], device_id=(s, peer), device_id_type=MESH)
        c.start()
        asent.append(c)

    for m in (0, 1):
        for h in (0, 1):
            recv(m, z2, h)
            send(2, m, z2, h)
    send(2, 2, s, 0, own=True)
    send(2, 2, s, 1, own=True)

    for peer in reach:
        recv_block(after, a_recv, peer)

    def norm(r, carry):
        rows = pl.ds(pl.multiple_of(r * 64, 64), 64)
        parts = [after[i, rows, :].astype(jnp.float32) for i in range(T)]
        square = (parts[0] * parts[0]).sum(-1, keepdims=True)
        for p in parts[1:]:
            square += (p * p).sum(-1, keepdims=True)
        inv = lax.rsqrt(square / D + norm_eps)
        for i in range(T):
            n = (parts[i] * inv * gain_ref[:, i * C:(i + 1) * C]).astype(jnp.bfloat16)
            for j in range(PER):
                normed[i * PER + j, rows, :] = n[:, j * K:(j + 1) * K]
        return carry

    lax.fori_loop(0, R // 64, norm, 0)

    TM = 128

    def gate_up(src, begin=False):
        def tile(r, carry):
            rows = pl.ds(pl.multiple_of(r * TM, TM), TM)
            a = normed[src, rows, :]
            for m, acc in ((0, ga), (1, ua)):
                value = dot(a, G[m, src])
                if begin:
                    acc[rows, :] = value
                else:
                    acc[rows, :] += value
            return carry
        lax.fori_loop(0, R // TM, tile, 0)

    local[0].wait()
    local[1].wait()
    gate_up(s, True)
    for src in (zm, zp, xp, z2):
        gate_up(src)
    for src in (zm_x, zp_x):
        for m in (0, 1):
            for h in (0, 1):
                recv(m, src, h)
        gate_up(src)
    recv(2, zm, 0)
    send(0, 2, zm, 0)
    recv(2, zp, 1)
    send(1, 2, zp, 1)
    for m in (0, 1):
        for h in (0, 1):
            recv(m, z2_x, h)
    gate_up(z2_x)

    def act(r, carry):
        rows = pl.ds(pl.multiple_of(r * 32, 32), 32)
        g = ga[rows, :]
        hidden[rows, :] = (g / (1.0 + jnp.exp(-g)) * ua[rows, :]).astype(jnp.bfloat16)
        return carry

    lax.fori_loop(0, R // 32, act, 0)

    def down_copy(src, h):
        owner = src // PER
        return owner, pltpu.make_async_remote_copy(
            src_ref=dsend.at[src, h], dst_ref=drecv.at[t, src % PER, h],
            send_sem=d_send.at[src, h], recv_sem=d_recv.at[t, src % PER, h],
            device_id=(s, owner), device_id_type=MESH)

    def down(src, h):
        value = dot(hidden[...], G[2, src, h * HK:(h + 1) * HK, :], NT).astype(jnp.bfloat16)
        owner, c = down_copy(src, h)

        @pl.when(owner != t)
        def _():
            dsend[src, h] = value
            c.start()

        @pl.when(owner == t)
        def _():
            drecv[t, src % PER, h] = value

    local[2].wait()
    for h in (0, 1):
        recv(2, xp, h)
        send(0, 2, xp, h)
        send(1, 2, xp, h)
        recv(2, z2, h)
        send(2, 2, z2, h)
        if h == 0:
            down(s, 0)
            down(s, 1)
    recv(2, zm, 1)
    recv(2, zp, 0)
    for src in (zm, zp, xp, z2):
        for h in (0, 1):
            down(src, h)
    for h in (0, 1):
        for src in (zm_x, zp_x, z2_x):
            recv(2, src, h)
            down(src, h)

    for i in range(PER):
        for h in (0, 1):
            for peer in reach:
                pltpu.make_async_remote_copy(
                    src_ref=drecv.at[peer, i, h], dst_ref=drecv.at[peer, i, h],
                    send_sem=d_send.at[0, 0], recv_sem=d_recv.at[peer, i, h],
                    device_id=(s, (t + 1) % T), device_id_type=MESH).wait_recv()
            total = drecv[0, i, h].astype(jnp.float32)
            for n in range(1, T):
                total += drecv[n, i, h].astype(jnp.float32)
            cols = slice((i * 2 + h) * HK, (i * 2 + h + 1) * HK)
            out_ref[:, cols] = (after[t, :, cols].astype(jnp.float32) + total).astype(jnp.bfloat16)

    for c in started + tails + psent + asent:
        c.wait_send()
    for src in range(S):
        for h in (0, 1):
            owner, c = down_copy(src, h)

            @pl.when(owner != t)
            def _():
                c.wait_send()


def fused(residual, queries, keys, values, documents, sinks, out_weight, norm_gain, gate_weight, up_weight, down_weight):
    S, T = lax.axis_size("sp"), lax.axis_size("tp")
    R, D = residual.shape
    F = gate_weight.shape[1]
    C, K = D // T, D // S
    blocks = R // WINDOW
    docs = jnp.broadcast_to(documents.reshape(blocks, 1, WINDOW), (blocks, 8, WINDOW)).reshape(blocks * 8, WINDOW)
    bf, f32 = jnp.bfloat16, jnp.float32
    vm, hbm = pl.BlockSpec(memory_space=pltpu.VMEM), pl.BlockSpec(memory_space=pl.ANY)
    dma = pltpu.SemaphoreType.DMA
    scratch = [
        pltpu.VMEM((3, S, K, F), bf),
        pltpu.VMEM((R + WINDOW, keys.shape[1]), bf),
        pltpu.VMEM((R + WINDOW, keys.shape[1]), bf),
        pltpu.VMEM((blocks * 8 + 8, WINDOW), jnp.int32),
        pltpu.VMEM((R, queries.shape[1]), bf),
        pltpu.VMEM((R, C), bf),
        pltpu.VMEM(out_weight.shape, bf),
        pltpu.VMEM((T, R, C), bf),
        pltpu.VMEM((T, R, C), bf),
        pltpu.VMEM((T, R, C), bf),
        pltpu.VMEM((S, R, K), bf),
        pltpu.VMEM((R, F), f32),
        pltpu.VMEM((R, F), f32),
        pltpu.VMEM((R, F), bf),
        pltpu.VMEM((S, 2, R, K // 2), bf),
        pltpu.VMEM((T, C // K, 2, R, K // 2), bf),
        dma((3, 14)), dma((3, S, 2)), dma((3,)), dma((3,)), dma((5,)),
        dma((T,)), dma((T,)), dma((T,)), dma((T,)), dma((S, 2)), dma((T, C // K, 2)),
    ]
    return pl.pallas_call(
        functools.partial(kernel, S, T),
        out_shape=jax.ShapeDtypeStruct((R, C), bf),
        in_specs=[hbm, vm, vm, vm, vm, pl.BlockSpec(memory_space=pltpu.SMEM), hbm, vm, hbm, hbm, hbm],
        out_specs=vm,
        scratch_shapes=scratch,
        compiler_params=pltpu.CompilerParams(
            collective_id=0, has_side_effects=True, vmem_limit_bytes=60 * 2**20),
    )(residual, queries, keys, values, docs, sinks, out_weight, norm_gain.reshape(1, D),
      gate_weight, up_weight, down_weight)


def ring_of_four_pairs(mesh):
    return mesh.shape["sp"] == 8 and mesh.shape["tp"] == 4


def solution(mesh):
    return jax.shard_map(
        fused if ring_of_four_pairs(mesh) else on_device,
        mesh=mesh,
        in_specs=(
            P("sp", None),
            P("sp", "tp"),
            P("sp", "tp"),
            P("sp", "tp"),
            P("sp"),
            P("tp"),
            P("tp", None),
            P(),
            P("sp", "tp"),
            P("sp", "tp"),
            P("sp", "tp"),
        ),
        out_specs=P("sp", "tp"),
        check_vma=False,
    )
```

```python
import functools

import jax
import jax.numpy as jnp
from jax import lax
from jax.experimental import pallas as pl
from jax.experimental.pallas import tpu as pltpu
from jax.sharding import PartitionSpec as P

HEAD_DIM = 64
WINDOW = 128
GROUP = 2


neg_big = -1e30
norm_eps = 1e-05


def from_behind(shard, axis, by):
    length = lax.axis_size(axis)
    pairs = [(i, i + by) for i in range(length) if 0 <= i + by < length]
    return lax.ppermute(shard, axis, pairs)


def attend(queries, keys, values, documents, sinks, tail_keys, tail_values, tail_docs, offset):
    rows_here = queries.shape[0]
    block_count = rows_here // WINDOW
    kv_here = keys.shape[1] // HEAD_DIM
    q_blocks = queries.reshape(block_count, WINDOW, kv_here, GROUP, HEAD_DIM)
    k_blocks = keys.reshape(block_count, WINDOW, kv_here, HEAD_DIM)
    v_blocks = values.reshape(block_count, WINDOW, kv_here, HEAD_DIM)
    k_prev = jnp.concatenate(
        [tail_keys.reshape(1, WINDOW, kv_here, HEAD_DIM), k_blocks[:-1]], axis=0
    )
    v_prev = jnp.concatenate(
        [tail_values.reshape(1, WINDOW, kv_here, HEAD_DIM), v_blocks[:-1]], axis=0
    )
    k_band = jnp.concatenate([k_prev, k_blocks], axis=1)
    v_band = jnp.concatenate([v_prev, v_blocks], axis=1)
    doc_own = documents.astype(jnp.float32).reshape(block_count, WINDOW)
    doc_prev = jnp.concatenate(
        [tail_docs.astype(jnp.float32).reshape(1, WINDOW), doc_own[:-1]], axis=0
    )
    doc_band = jnp.concatenate([doc_prev, doc_own], axis=1)
    row_idx = jnp.arange(WINDOW, dtype=jnp.int32)
    col_idx = jnp.arange(2 * WINDOW, dtype=jnp.int32)
    first = offset + jnp.arange(block_count, dtype=jnp.int32) * WINDOW
    q_pos = first[:, None] + row_idx[None, :]
    k_pos = first[:, None] - WINDOW + col_idx[None, :]
    distance = q_pos[:, :, None] - k_pos[:, None, :]
    visible = (
        (distance >= 0)
        & (distance < WINDOW)
        & (k_pos[:, None, :] >= 0)
        & (doc_own[:, :, None] == doc_band[:, None, :])
    )
    scores = jnp.einsum(
        "nikgd,njkd->nkgij", q_blocks, k_band, preferred_element_type=jnp.float32
    ) * HEAD_DIM ** (-0.5)
    scores = jnp.where(visible[:, None, None], scores, neg_big)
    sink_logit = sinks.reshape(1, kv_here, GROUP, 1, 1)
    row_max = jnp.maximum(scores.max(-1, keepdims=True), sink_logit)
    expo = jnp.where(visible[:, None, None], jnp.exp(scores - row_max), 0.0)
    denom_sum = expo.sum(-1, keepdims=True) + jnp.exp(sink_logit - row_max)
    weights = (expo / denom_sum).astype(jnp.bfloat16)
    mixed = jnp.einsum("nkgij,njkd->nikgd", weights, v_band, preferred_element_type=jnp.float32)
    return mixed.reshape(rows_here, kv_here * GROUP * HEAD_DIM).astype(jnp.bfloat16)


def on_device(
    residual,
    queries,
    keys,
    values,
    documents,
    sinks,
    out_weight,
    norm_gain,
    gate_weight,
    up_weight,
    down_weight,
):
    rows_here = queries.shape[0]
    offset = lax.axis_index("sp") * rows_here
    doc_tail = documents[rows_here - WINDOW :].astype(jnp.bfloat16)
    tail_keys, tail_values, tail_docs = from_behind(
        (keys[rows_here - WINDOW :], values[rows_here - WINDOW :], doc_tail), "sp", 1
    )
    attended = attend(
        queries, keys, values, documents, sinks, tail_keys, tail_values, tail_docs, offset
    )
    model_width = residual.shape[1]
    col_count = model_width // lax.axis_size("tp")
    col_first = lax.axis_index("tp") * col_count
    full_term = jnp.dot(attended, out_weight, preferred_element_type=jnp.float32)
    projected = lax.psum(full_term.astype(jnp.bfloat16), "tp").astype(jnp.float32)
    after_full = (residual.astype(jnp.float32) + projected).astype(jnp.bfloat16)
    after_f = after_full.astype(jnp.float32)
    inv_rms = lax.rsqrt(jnp.mean(after_f * after_f, axis=1, keepdims=True) + norm_eps)
    normed = (after_f * inv_rms * norm_gain[None, :]).astype(jnp.bfloat16)
    after = lax.dynamic_slice_in_dim(after_full, col_first, col_count, 1)
    gate_act = jnp.dot(
        normed,
        lax.all_gather(gate_weight, "sp", axis=0, tiled=True),
        preferred_element_type=jnp.float32,
    )
    up_act = jnp.dot(
        normed,
        lax.all_gather(up_weight, "sp", axis=0, tiled=True),
        preferred_element_type=jnp.float32,
    )
    down_full = lax.all_gather(down_weight, "sp", axis=0, tiled=True)
    hidden = (jax.nn.silu(gate_act) * up_act).astype(jnp.bfloat16)
    summed = lax.psum_scatter(
        lax.dot_general(
            down_full, hidden, (((1,), (1,)), ((), ())), preferred_element_type=jnp.float32
        ).astype(jnp.bfloat16),
        "tp",
        scatter_dimension=0,
        tiled=True,
    ).astype(jnp.float32)
    return (after.astype(jnp.float32) + summed.T).astype(jnp.bfloat16)


MESH = pl.DeviceIdType.MESH
NT = (((1,), (1,)), ((), ()))


def dot(a, b, dims=(((1,), (0,)), ((), ()))):
    return lax.dot_general(a, b, dims, preferred_element_type=jnp.float32)


def kernel(
    S, T,
    res_hbm, q_ref, k_ref, v_ref, doc_ref, sink_ref, ow_hbm, gain_ref, g_hbm, u_hbm, d_hbm,
    out_ref,
    G, kx, vx, dx, att, res_v, ow_v, psend, precv, after, normed, ga, ua, hidden, dsend, drecv,
    w_send, w_recv, tail_send, tail_recv, loc, p_send, p_recv, a_send, a_recv, d_send, d_recv,
):
    s = lax.axis_index("sp")
    t = lax.axis_index("tp")
    R = q_ref.shape[0]
    D = gain_ref.shape[1]
    C = D // T
    K = D // S
    F = g_hbm.shape[1]
    HK = K // 2
    PER = C // K
    z, x = s // 2, s % 2
    up, down_z = (z + 1) % 4, (z + 3) % 4
    nb_z = z + 1 - 2 * (z % 2)
    f1_z = 2 - z // 2
    f2_z = 3 - 3 * (z // 2)
    zp, zm, xp = up * 2 + x, down_z * 2 + x, z * 2 + 1 - x
    nb, f1, f2 = nb_z * 2 + x, f1_z * 2 + x, f2_z * 2 + x
    nb_x, f1_x, f2_x = nb_z * 2 + 1 - x, f1_z * 2 + 1 - x, f2_z * 2 + 1 - x
    far = ((z + 2) % 4) * 2 + x
    end = (3 - z) * 2 + x
    has_up, has_down = z < 3, z > 0
    after_s = (s + 1) % S
    before_s = (s + S - 1) % S

    weights = (g_hbm, u_hbm, d_hbm)
    local = [
        pltpu.make_async_copy(weights[m], G.at[m, s], loc.at[m]) for m in range(3)
    ]
    local.append(pltpu.make_async_copy(ow_hbm, ow_v, loc.at[3]))
    local.append(pltpu.make_async_copy(
        res_hbm.at[:, pl.ds(pl.multiple_of(t * C, C), C)], res_v, loc.at[4]))
    for c in (local[3], local[4], local[0], local[1], local[2]):
        c.start()

    barrier = pltpu.get_barrier_semaphore()
    peers = [(zp, t), (zm, t), (xp, t), (after_s, t), (before_s, t)]
    peers += [(s, (t + d) % T) for d in range(1, T)]
    for p in peers:
        pl.semaphore_signal(barrier, inc=1, device_id=p, device_id_type=MESH)
    pl.semaphore_wait(barrier, len(peers))

    started = []

    tails = []
    for i, (a, b) in enumerate((
        (k_ref.at[pl.ds(R - WINDOW, WINDOW)], kx.at[pl.ds(0, WINDOW)]),
        (v_ref.at[pl.ds(R - WINDOW, WINDOW)], vx.at[pl.ds(0, WINDOW)]),
        (doc_ref.at[pl.ds(doc_ref.shape[0] - 8, 8)], dx.at[pl.ds(0, 8)]),
    )):
        c = pltpu.make_async_remote_copy(
            src_ref=a, dst_ref=b, send_sem=tail_send.at[i], recv_sem=tail_recv.at[i],
            device_id=(after_s, t), device_id_type=MESH)
        c.start()
        tails.append(c)

    target = (zp, zm, xp, nb)
    count = [0, 0, 0, 0]

    def when(cond, f):
        if cond is None:
            f()
        else:
            pl.when(cond)(f)

    def send(link, m, src, h, own=False, cond=None):
        part = pl.ds(h * HK, HK)
        place = G.at[m, src, part]
        c = pltpu.make_async_remote_copy(
            src_ref=weights[m].at[part] if own else place, dst_ref=place,
            send_sem=w_send.at[link, count[link]], recv_sem=w_recv.at[m, src, h],
            device_id=(target[link], t), device_id_type=MESH)
        count[link] += 1
        when(cond, c.start)
        started.append((cond, c))

    def recv(m, src, h, cond=None):
        place = G.at[m, src, pl.ds(h * HK, HK)]
        c = pltpu.make_async_remote_copy(
            src_ref=place, dst_ref=place, send_sem=w_send.at[0, 0],
            recv_sem=w_recv.at[m, src, h], device_id=(xp, t), device_id_type=MESH)
        when(cond, c.wait_recv)

    GU = ((0, 0), (0, 1), (1, 0), (1, 1))
    DN = ((2, 0), (2, 1))

    def own_z(units):
        for m, h in units:
            send(0, m, s, h, own=True, cond=has_up)
            send(1, m, s, h, own=True, cond=has_down)

    def own_x(units):
        for m, h in units:
            send(2, m, s, h, own=True)

    def near(units):
        for m, h in units:
            recv(m, zp, h, has_up)
            send(1, m, zp, h, cond=has_up & has_down)
            recv(m, zm, h, has_down)
            send(0, m, zm, h, cond=has_up & has_down)
            if h == 1:
                send(2, m, nb, h)

    def middle(units):
        for m, h in units:
            recv(m, far, h)
            send(1, m, far, h, cond=z == 1)
            send(0, m, far, h, cond=z == 2)
            send(2, m, f1, h)

    def farthest(units):
        for m, h in units:
            recv(m, end, h, (z == 0) | (z == 3))
            send(2, m, f2, h)

    def extra(units):
        for m, h in units:
            recv(m, xp, h)
            if h == 0:
                send(3, m, xp, h)

    for m, h in GU:
        send(0, m, s, h, own=True, cond=has_up)
        send(1, m, s, h, own=True, cond=has_down)
        send(2, m, s, h, own=True)

    kx[pl.ds(WINDOW, R), :] = k_ref[...]
    vx[pl.ds(WINDOW, R), :] = v_ref[...]
    dx[pl.ds(8, doc_ref.shape[0]), :] = doc_ref[...]
    for c in tails:
        c.wait_recv()
    heads = q_ref.shape[1] // HEAD_DIM

    def block(b, carry):
        rows = pl.ds(pl.multiple_of(b * WINDOW, WINDOW), WINDOW)
        band = pl.ds(pl.multiple_of(b * WINDOW, WINDOW), 2 * WINDOW)
        prev = dx[pl.ds(pl.multiple_of(b * 8, 8), 8), :][0:1].astype(jnp.float32)
        own = dx[pl.ds(pl.multiple_of(b * 8 + 8, 8), 8), :][0:1].astype(jnp.float32)
        doc_q = jnp.broadcast_to(own, (WINDOW, WINDOW)).T
        i = lax.broadcasted_iota(jnp.int32, (WINDOW, WINDOW), 0)
        j = lax.broadcasted_iota(jnp.int32, (WINDOW, WINDOW), 1)
        first = s * R + b * WINDOW - WINDOW
        see_prev = (j > i) & (doc_q == prev) & (first + j >= 0)
        see_own = (j <= i) & (doc_q == own)
        visible = jnp.concatenate(
            [see_prev.astype(jnp.float32), see_own.astype(jnp.float32)], axis=1) > 0.5
        for h in range(heads):
            kv = h // GROUP
            cols = slice(kv * HEAD_DIM, (kv + 1) * HEAD_DIM)
            q = q_ref[rows, h * HEAD_DIM:(h + 1) * HEAD_DIM]
            scores = dot(q, kx[band, cols], NT) * HEAD_DIM ** (-0.5)
            scores = jnp.where(visible, scores, neg_big)
            sink = sink_ref[h]
            row_max = jnp.maximum(scores.max(-1, keepdims=True), sink)
            expo = jnp.where(visible, jnp.exp(scores - row_max), 0.0)
            total = expo.sum(-1, keepdims=True) + jnp.exp(sink - row_max)
            w = (expo / total).astype(jnp.bfloat16)
            att[rows, h * HEAD_DIM:(h + 1) * HEAD_DIM] = dot(w, vx[band, cols]).astype(jnp.bfloat16)
        return carry

    lax.fori_loop(0, R // WINDOW, block, 0)

    local[3].wait()
    reach = [(t + d) % T for d in (2, 1, 3)]
    psent = []
    for n, owner in enumerate(reach + [t]):
        cols = pl.ds(pl.multiple_of(owner * C, C), C)
        value = dot(att[...], ow_v[:, cols]).astype(jnp.bfloat16)
        if n == T - 1:
            precv[t] = value
        else:
            psend[owner] = value
            c = pltpu.make_async_remote_copy(
                src_ref=psend.at[owner], dst_ref=precv.at[t], send_sem=p_send.at[n],
                recv_sem=p_recv.at[t], device_id=(s, owner), device_id_type=MESH)
            c.start()
            psent.append(c)

    def recv_block(buf, sems, source):
        pltpu.make_async_remote_copy(
            src_ref=buf.at[source], dst_ref=buf.at[source], send_sem=p_send.at[0],
            recv_sem=sems.at[source], device_id=(s, (t + 1) % T), device_id_type=MESH).wait_recv()

    near(GU)

    local[4].wait()
    for owner in reach:
        recv_block(precv, p_recv, owner)
    total = precv[0].astype(jnp.float32)
    for i in range(1, T):
        total += precv[i].astype(jnp.float32)
    after[t] = (res_v[...].astype(jnp.float32) + total).astype(jnp.bfloat16)
    asent = []
    for n, peer in enumerate(reach):
        c = pltpu.make_async_remote_copy(
            src_ref=after.at[t], dst_ref=after.at[t], send_sem=a_send.at[n],
            recv_sem=a_recv.at[t], device_id=(s, peer), device_id_type=MESH)
        c.start()
        asent.append(c)

    middle(GU)
    extra(GU)
    own_z(DN)

    for peer in reach:
        recv_block(after, a_recv, peer)

    def norm(r, carry):
        rows = pl.ds(pl.multiple_of(r * 64, 64), 64)
        parts = [after[i, rows, :].astype(jnp.float32) for i in range(T)]
        square = (parts[0] * parts[0]).sum(-1, keepdims=True)
        for p in parts[1:]:
            square += (p * p).sum(-1, keepdims=True)
        inv = lax.rsqrt(square / D + norm_eps)
        for i in range(T):
            n = (parts[i] * inv * gain_ref[:, i * C:(i + 1) * C]).astype(jnp.bfloat16)
            for j in range(PER):
                normed[i * PER + j, rows, :] = n[:, j * K:(j + 1) * K]
        return carry

    lax.fori_loop(0, R // 64, norm, 0)

    TM = 128

    def gate_up(src, begin=False):
        def tile(r, carry):
            rows = pl.ds(pl.multiple_of(r * TM, TM), TM)
            a = normed[src, rows, :]
            for m, acc in ((0, ga), (1, ua)):
                value = dot(a, G[m, src])
                if begin:
                    acc[rows, :] = value
                else:
                    acc[rows, :] += value
            return carry
        lax.fori_loop(0, R // TM, tile, 0)

    local[0].wait()
    local[1].wait()
    gate_up(s, True)
    gate_up(nb)
    farthest(GU[:2])
    gate_up(xp)
    gate_up(f1)
    farthest(GU[2:])
    own_x(DN)
    gate_up(f2)
    for src in (nb_x, f1_x, f2_x):
        for m, h in GU:
            recv(m, src, h)
        gate_up(src)

    def act(r, carry):
        rows = pl.ds(pl.multiple_of(r * 32, 32), 32)
        g = ga[rows, :]
        hidden[rows, :] = (g / (1.0 + jnp.exp(-g)) * ua[rows, :]).astype(jnp.bfloat16)
        return carry

    lax.fori_loop(0, R // 32, act, 0)

    def down_copy(src, h):
        owner = src // PER
        return owner, pltpu.make_async_remote_copy(
            src_ref=dsend.at[src, h], dst_ref=drecv.at[t, src % PER, h],
            send_sem=d_send.at[src, h], recv_sem=d_recv.at[t, src % PER, h],
            device_id=(s, owner), device_id_type=MESH)

    def down(src, h):
        value = dot(hidden[...], G[2, src, h * HK:(h + 1) * HK, :], NT).astype(jnp.bfloat16)
        owner, c = down_copy(src, h)

        @pl.when(owner != t)
        def _():
            dsend[src, h] = value
            c.start()

        @pl.when(owner == t)
        def _():
            drecv[t, src % PER, h] = value

    local[2].wait()
    near(DN)
    down(s, 0)
    down(s, 1)
    down(nb, 0)
    down(nb, 1)
    middle(DN)
    extra(DN)
    for src in (xp, f1):
        for h in (0, 1):
            down(src, h)
    for h in (1, 0):
        if h == 0:
            farthest(DN)
        recv(2, nb_x, h)
        down(nb_x, h)
    for src in (f2, f1_x, f2_x):
        for h in (0, 1):
            if src is not f2:
                recv(2, src, h)
            down(src, h)

    for i in range(PER):
        for h in (0, 1):
            for peer in reach:
                pltpu.make_async_remote_copy(
                    src_ref=drecv.at[peer, i, h], dst_ref=drecv.at[peer, i, h],
                    send_sem=d_send.at[0, 0], recv_sem=d_recv.at[peer, i, h],
                    device_id=(s, (t + 1) % T), device_id_type=MESH).wait_recv()
            total = drecv[0, i, h].astype(jnp.float32)
            for n in range(1, T):
                total += drecv[n, i, h].astype(jnp.float32)
            cols = slice((i * 2 + h) * HK, (i * 2 + h + 1) * HK)
            out_ref[:, cols] = (after[t, :, cols].astype(jnp.float32) + total).astype(jnp.bfloat16)

    for cond, c in started:
        when(cond, c.wait_send)
    for c in tails + psent + asent:
        c.wait_send()
    for src in range(S):
        for h in (0, 1):
            owner, c = down_copy(src, h)

            @pl.when(owner != t)
            def _():
                c.wait_send()


def fused(residual, queries, keys, values, documents, sinks, out_weight, norm_gain, gate_weight, up_weight, down_weight):
    S, T = lax.axis_size("sp"), lax.axis_size("tp")
    R, D = residual.shape
    F = gate_weight.shape[1]
    C, K = D // T, D // S
    blocks = R // WINDOW
    docs = jnp.broadcast_to(documents.reshape(blocks, 1, WINDOW), (blocks, 8, WINDOW)).reshape(blocks * 8, WINDOW)
    bf, f32 = jnp.bfloat16, jnp.float32
    vm, hbm = pl.BlockSpec(memory_space=pltpu.VMEM), pl.BlockSpec(memory_space=pl.ANY)
    dma = pltpu.SemaphoreType.DMA
    scratch = [
        pltpu.VMEM((3, S, K, F), bf),
        pltpu.VMEM((R + WINDOW, keys.shape[1]), bf),
        pltpu.VMEM((R + WINDOW, keys.shape[1]), bf),
        pltpu.VMEM((blocks * 8 + 8, WINDOW), jnp.int32),
        pltpu.VMEM((R, queries.shape[1]), bf),
        pltpu.VMEM((R, C), bf),
        pltpu.VMEM(out_weight.shape, bf),
        pltpu.VMEM((T, R, C), bf),
        pltpu.VMEM((T, R, C), bf),
        pltpu.VMEM((T, R, C), bf),
        pltpu.VMEM((S, R, K), bf),
        pltpu.VMEM((R, F), f32),
        pltpu.VMEM((R, F), f32),
        pltpu.VMEM((R, F), bf),
        pltpu.VMEM((S, 2, R, K // 2), bf),
        pltpu.VMEM((T, C // K, 2, R, K // 2), bf),
        dma((4, 21)), dma((3, S, 2)), dma((3,)), dma((3,)), dma((5,)),
        dma((T,)), dma((T,)), dma((T,)), dma((T,)), dma((S, 2)), dma((T, C // K, 2)),
    ]
    return pl.pallas_call(
        functools.partial(kernel, S, T),
        out_shape=jax.ShapeDtypeStruct((R, C), bf),
        in_specs=[hbm, vm, vm, vm, vm, pl.BlockSpec(memory_space=pltpu.SMEM), hbm, vm, hbm, hbm, hbm],
        out_specs=vm,
        scratch_shapes=scratch,
        compiler_params=pltpu.CompilerParams(
            collective_id=0, has_side_effects=True, vmem_limit_bytes=60 * 2**20),
    )(residual, queries, keys, values, docs, sinks, out_weight, norm_gain.reshape(1, D),
      gate_weight, up_weight, down_weight)


def line_of_four_pairs(mesh):
    return mesh.shape["sp"] == 8 and mesh.shape["tp"] == 4


def solution(mesh):
    return jax.shard_map(
        fused if line_of_four_pairs(mesh) else on_device,
        mesh=mesh,
        in_specs=(
            P("sp", None),
            P("sp", "tp"),
            P("sp", "tp"),
            P("sp", "tp"),
            P("sp"),
            P("tp"),
            P("tp", None),
            P(),
            P("sp", "tp"),
            P("sp", "tp"),
            P("sp", "tp"),
        ),
        out_specs=P("sp", "tp"),
        check_vma=False,
    )
```

```python
import functools

import jax
import jax.numpy as jnp
from jax import lax
from jax.experimental import pallas as pl
from jax.experimental.pallas import tpu as pltpu
from jax.sharding import PartitionSpec as P

HEAD_DIM = 64
WINDOW = 128
GROUP = 2


neg_big = -1e30
norm_eps = 1e-05


def from_behind(shard, axis, by):
    length = lax.axis_size(axis)
    pairs = [(i, i + by) for i in range(length) if 0 <= i + by < length]
    return lax.ppermute(shard, axis, pairs)


def attend(queries, keys, values, documents, sinks, tail_keys, tail_values, tail_docs, offset):
    rows_here = queries.shape[0]
    block_count = rows_here // WINDOW
    kv_here = keys.shape[1] // HEAD_DIM
    q_blocks = queries.reshape(block_count, WINDOW, kv_here, GROUP, HEAD_DIM)
    k_blocks = keys.reshape(block_count, WINDOW, kv_here, HEAD_DIM)
    v_blocks = values.reshape(block_count, WINDOW, kv_here, HEAD_DIM)
    k_prev = jnp.concatenate(
        [tail_keys.reshape(1, WINDOW, kv_here, HEAD_DIM), k_blocks[:-1]], axis=0
    )
    v_prev = jnp.concatenate(
        [tail_values.reshape(1, WINDOW, kv_here, HEAD_DIM), v_blocks[:-1]], axis=0
    )
    k_band = jnp.concatenate([k_prev, k_blocks], axis=1)
    v_band = jnp.concatenate([v_prev, v_blocks], axis=1)
    doc_own = documents.astype(jnp.float32).reshape(block_count, WINDOW)
    doc_prev = jnp.concatenate(
        [tail_docs.astype(jnp.float32).reshape(1, WINDOW), doc_own[:-1]], axis=0
    )
    doc_band = jnp.concatenate([doc_prev, doc_own], axis=1)
    row_idx = jnp.arange(WINDOW, dtype=jnp.int32)
    col_idx = jnp.arange(2 * WINDOW, dtype=jnp.int32)
    first = offset + jnp.arange(block_count, dtype=jnp.int32) * WINDOW
    q_pos = first[:, None] + row_idx[None, :]
    k_pos = first[:, None] - WINDOW + col_idx[None, :]
    distance = q_pos[:, :, None] - k_pos[:, None, :]
    visible = (
        (distance >= 0)
        & (distance < WINDOW)
        & (k_pos[:, None, :] >= 0)
        & (doc_own[:, :, None] == doc_band[:, None, :])
    )
    scores = jnp.einsum(
        "nikgd,njkd->nkgij", q_blocks, k_band, preferred_element_type=jnp.float32
    ) * HEAD_DIM ** (-0.5)
    scores = jnp.where(visible[:, None, None], scores, neg_big)
    sink_logit = sinks.reshape(1, kv_here, GROUP, 1, 1)
    row_max = jnp.maximum(scores.max(-1, keepdims=True), sink_logit)
    expo = jnp.where(visible[:, None, None], jnp.exp(scores - row_max), 0.0)
    denom_sum = expo.sum(-1, keepdims=True) + jnp.exp(sink_logit - row_max)
    weights = (expo / denom_sum).astype(jnp.bfloat16)
    mixed = jnp.einsum("nkgij,njkd->nikgd", weights, v_band, preferred_element_type=jnp.float32)
    return mixed.reshape(rows_here, kv_here * GROUP * HEAD_DIM).astype(jnp.bfloat16)


def on_device(
    residual,
    queries,
    keys,
    values,
    documents,
    sinks,
    out_weight,
    norm_gain,
    gate_weight,
    up_weight,
    down_weight,
):
    rows_here = queries.shape[0]
    offset = lax.axis_index("sp") * rows_here
    doc_tail = documents[rows_here - WINDOW :].astype(jnp.bfloat16)
    tail_keys, tail_values, tail_docs = from_behind(
        (keys[rows_here - WINDOW :], values[rows_here - WINDOW :], doc_tail), "sp", 1
    )
    attended = attend(
        queries, keys, values, documents, sinks, tail_keys, tail_values, tail_docs, offset
    )
    model_width = residual.shape[1]
    col_count = model_width // lax.axis_size("tp")
    col_first = lax.axis_index("tp") * col_count
    full_term = jnp.dot(attended, out_weight, preferred_element_type=jnp.float32)
    projected = lax.psum(full_term.astype(jnp.bfloat16), "tp").astype(jnp.float32)
    after_full = (residual.astype(jnp.float32) + projected).astype(jnp.bfloat16)
    after_f = after_full.astype(jnp.float32)
    inv_rms = lax.rsqrt(jnp.mean(after_f * after_f, axis=1, keepdims=True) + norm_eps)
    normed = (after_f * inv_rms * norm_gain[None, :]).astype(jnp.bfloat16)
    after = lax.dynamic_slice_in_dim(after_full, col_first, col_count, 1)
    gate_act = jnp.dot(
        normed,
        lax.all_gather(gate_weight, "sp", axis=0, tiled=True),
        preferred_element_type=jnp.float32,
    )
    up_act = jnp.dot(
        normed,
        lax.all_gather(up_weight, "sp", axis=0, tiled=True),
        preferred_element_type=jnp.float32,
    )
    down_full = lax.all_gather(down_weight, "sp", axis=0, tiled=True)
    hidden = (jax.nn.silu(gate_act) * up_act).astype(jnp.bfloat16)
    summed = lax.psum_scatter(
        lax.dot_general(
            down_full, hidden, (((1,), (1,)), ((), ())), preferred_element_type=jnp.float32
        ).astype(jnp.bfloat16),
        "tp",
        scatter_dimension=0,
        tiled=True,
    ).astype(jnp.float32)
    return (after.astype(jnp.float32) + summed.T).astype(jnp.bfloat16)


MESH = pl.DeviceIdType.MESH
NT = (((1,), (1,)), ((), ()))


def dot(a, b, dims=(((1,), (0,)), ((), ()))):
    return lax.dot_general(a, b, dims, preferred_element_type=jnp.float32)


def kernel(
    S, T,
    res_hbm, q_ref, k_ref, v_ref, doc_ref, sink_ref, ow_hbm, gain_ref, g_hbm, u_hbm, d_hbm,
    out_ref,
    G, kx, vx, dx, att, res_v, ow_v, psend, precv, after, normed, ga, ua, hidden, dsend, drecv,
    w_send, w_recv, tail_send, tail_recv, loc, p_send, p_recv, a_send, a_recv, d_send, d_recv,
):
    s = lax.axis_index("sp")
    t = lax.axis_index("tp")
    R = q_ref.shape[0]
    D = gain_ref.shape[1]
    C = D // T
    K = D // S
    F = g_hbm.shape[1]
    HK = K // 2
    PER = C // K
    z, x = s // 2, s % 2
    up, down_z = (z + 1) % 4, (z + 3) % 4
    nb_z = z + 1 - 2 * (z % 2)
    f1_z = 2 - z // 2
    f2_z = 3 - 3 * (z // 2)
    zp, zm, xp = up * 2 + x, down_z * 2 + x, z * 2 + 1 - x
    nb, f1, f2 = nb_z * 2 + x, f1_z * 2 + x, f2_z * 2 + x
    nb_x, f1_x, f2_x = nb_z * 2 + 1 - x, f1_z * 2 + 1 - x, f2_z * 2 + 1 - x
    far = ((z + 2) % 4) * 2 + x
    end = (3 - z) * 2 + x
    has_up, has_down = z < 3, z > 0
    after_s = (s + 1) % S
    before_s = (s + S - 1) % S

    weights = (g_hbm, u_hbm, d_hbm)
    local = [
        pltpu.make_async_copy(weights[m], G.at[m, s], loc.at[m]) for m in range(3)
    ]
    local.append(pltpu.make_async_copy(ow_hbm, ow_v, loc.at[3]))
    local.append(pltpu.make_async_copy(
        res_hbm.at[:, pl.ds(pl.multiple_of(t * C, C), C)], res_v, loc.at[4]))
    for c in (local[3], local[4], local[0], local[1], local[2]):
        c.start()

    barrier = pltpu.get_barrier_semaphore()
    peers = [(zp, t), (zm, t), (xp, t), (after_s, t), (before_s, t)]
    peers += [(s, (t + d) % T) for d in range(1, T)]
    for p in peers:
        pl.semaphore_signal(barrier, inc=1, device_id=p, device_id_type=MESH)
    pl.semaphore_wait(barrier, len(peers))

    started = []

    tails = []
    for i, (a, b) in enumerate((
        (k_ref.at[pl.ds(R - WINDOW, WINDOW)], kx.at[pl.ds(0, WINDOW)]),
        (v_ref.at[pl.ds(R - WINDOW, WINDOW)], vx.at[pl.ds(0, WINDOW)]),
        (doc_ref.at[pl.ds(doc_ref.shape[0] - 8, 8)], dx.at[pl.ds(0, 8)]),
    )):
        c = pltpu.make_async_remote_copy(
            src_ref=a, dst_ref=b, send_sem=tail_send.at[i], recv_sem=tail_recv.at[i],
            device_id=(after_s, t), device_id_type=MESH)
        c.start()
        tails.append(c)

    target = (zp, zm, xp, nb)
    count = [0, 0, 0, 0]

    def when(cond, f):
        if cond is None:
            f()
        else:
            pl.when(cond)(f)

    def send(link, m, src, h, own=False, cond=None):
        part = pl.ds(h * HK, HK)
        place = G.at[m, src, part]
        c = pltpu.make_async_remote_copy(
            src_ref=weights[m].at[part] if own else place, dst_ref=place,
            send_sem=w_send.at[link, count[link]], recv_sem=w_recv.at[m, src, h],
            device_id=(target[link], t), device_id_type=MESH)
        count[link] += 1
        when(cond, c.start)
        started.append((cond, c))

    def recv(m, src, h, cond=None):
        place = G.at[m, src, pl.ds(h * HK, HK)]
        c = pltpu.make_async_remote_copy(
            src_ref=place, dst_ref=place, send_sem=w_send.at[0, 0],
            recv_sem=w_recv.at[m, src, h], device_id=(xp, t), device_id_type=MESH)
        when(cond, c.wait_recv)

    GU = ((0, 0), (0, 1), (1, 0), (1, 1))
    DN = ((2, 0), (2, 1))

    def own_z(units):
        for m, h in units:
            send(0, m, s, h, own=True, cond=has_up)
            send(1, m, s, h, own=True, cond=has_down)

    def own_x(units):
        for m, h in units:
            send(2, m, s, h, own=True)

    def near(units):
        for m, h in units:
            recv(m, zp, h, has_up)
            send(1, m, zp, h, cond=has_up & has_down)
            recv(m, zm, h, has_down)
            send(0, m, zm, h, cond=has_up & has_down)
            if h == 1:
                send(2, m, nb, h)

    def middle(units):
        for m, h in units:
            recv(m, far, h)
            send(1, m, far, h, cond=z == 1)
            send(0, m, far, h, cond=z == 2)
            send(2, m, f1, h)

    def farthest(units):
        for m, h in units:
            recv(m, end, h, (z == 0) | (z == 3))
            send(2, m, f2, h)

    def extra(units):
        for m, h in units:
            recv(m, xp, h)
            if h == 0:
                send(3, m, xp, h)

    for m, h in GU:
        send(0, m, s, h, own=True, cond=has_up)
        send(1, m, s, h, own=True, cond=has_down)
        send(2, m, s, h, own=True)

    kx[pl.ds(WINDOW, R), :] = k_ref[...]
    vx[pl.ds(WINDOW, R), :] = v_ref[...]
    dx[pl.ds(8, doc_ref.shape[0]), :] = doc_ref[...]
    for c in tails:
        c.wait_recv()
    heads = q_ref.shape[1] // HEAD_DIM

    def block(b, carry):
        rows = pl.ds(pl.multiple_of(b * WINDOW, WINDOW), WINDOW)
        band = pl.ds(pl.multiple_of(b * WINDOW, WINDOW), 2 * WINDOW)
        prev = dx[pl.ds(pl.multiple_of(b * 8, 8), 8), :][0:1].astype(jnp.float32)
        own = dx[pl.ds(pl.multiple_of(b * 8 + 8, 8), 8), :][0:1].astype(jnp.float32)
        doc_q = jnp.broadcast_to(own, (WINDOW, WINDOW)).T
        i = lax.broadcasted_iota(jnp.int32, (WINDOW, WINDOW), 0)
        j = lax.broadcasted_iota(jnp.int32, (WINDOW, WINDOW), 1)
        first = s * R + b * WINDOW - WINDOW
        see_prev = (j > i) & (doc_q == prev) & (first + j >= 0)
        see_own = (j <= i) & (doc_q == own)
        visible = jnp.concatenate(
            [see_prev.astype(jnp.float32), see_own.astype(jnp.float32)], axis=1) > 0.5
        for h in range(heads):
            kv = h // GROUP
            cols = slice(kv * HEAD_DIM, (kv + 1) * HEAD_DIM)
            q = q_ref[rows, h * HEAD_DIM:(h + 1) * HEAD_DIM]
            scores = dot(q, kx[band, cols], NT) * HEAD_DIM ** (-0.5)
            scores = jnp.where(visible, scores, neg_big)
            sink = sink_ref[h]
            row_max = jnp.maximum(scores.max(-1, keepdims=True), sink)
            expo = jnp.where(visible, jnp.exp(scores - row_max), 0.0)
            total = expo.sum(-1, keepdims=True) + jnp.exp(sink - row_max)
            w = (expo / total).astype(jnp.bfloat16)
            att[rows, h * HEAD_DIM:(h + 1) * HEAD_DIM] = dot(w, vx[band, cols]).astype(jnp.bfloat16)
        return carry

    lax.fori_loop(0, R // WINDOW, block, 0)

    local[3].wait()
    reach = [(t + d) % T for d in (2, 1, 3)]
    psent = []
    for n, owner in enumerate(reach + [t]):
        cols = pl.ds(pl.multiple_of(owner * C, C), C)
        value = dot(att[...], ow_v[:, cols]).astype(jnp.bfloat16)
        if n == T - 1:
            precv[t] = value
        else:
            psend[owner] = value
            c = pltpu.make_async_remote_copy(
                src_ref=psend.at[owner], dst_ref=precv.at[t], send_sem=p_send.at[n],
                recv_sem=p_recv.at[t], device_id=(s, owner), device_id_type=MESH)
            c.start()
            psent.append(c)

    def recv_block(buf, sems, source):
        pltpu.make_async_remote_copy(
            src_ref=buf.at[source], dst_ref=buf.at[source], send_sem=p_send.at[0],
            recv_sem=sems.at[source], device_id=(s, (t + 1) % T), device_id_type=MESH).wait_recv()

    near(GU)

    local[4].wait()
    for owner in reach:
        recv_block(precv, p_recv, owner)
    total = precv[0].astype(jnp.float32)
    for i in range(1, T):
        total += precv[i].astype(jnp.float32)
    after[t] = (res_v[...].astype(jnp.float32) + total).astype(jnp.bfloat16)
    asent = []
    for n, peer in enumerate(reach):
        c = pltpu.make_async_remote_copy(
            src_ref=after.at[t], dst_ref=after.at[t], send_sem=a_send.at[n],
            recv_sem=a_recv.at[t], device_id=(s, peer), device_id_type=MESH)
        c.start()
        asent.append(c)

    middle(GU)
    extra(GU)
    own_z(DN)
    farthest(GU[:2])

    for peer in reach:
        recv_block(after, a_recv, peer)

    def norm(r, carry):
        rows = pl.ds(pl.multiple_of(r * 64, 64), 64)
        parts = [after[i, rows, :].astype(jnp.float32) for i in range(T)]
        square = (parts[0] * parts[0]).sum(-1, keepdims=True)
        for p in parts[1:]:
            square += (p * p).sum(-1, keepdims=True)
        inv = lax.rsqrt(square / D + norm_eps)
        for i in range(T):
            n = (parts[i] * inv * gain_ref[:, i * C:(i + 1) * C]).astype(jnp.bfloat16)
            for j in range(PER):
                normed[i * PER + j, rows, :] = n[:, j * K:(j + 1) * K]
        return carry

    lax.fori_loop(0, R // 64, norm, 0)

    TM = 128

    def gate_up(src, begin=False):
        def tile(r, carry):
            rows = pl.ds(pl.multiple_of(r * TM, TM), TM)
            a = normed[src, rows, :]
            for m, acc in ((0, ga), (1, ua)):
                value = dot(a, G[m, src])
                if begin:
                    acc[rows, :] = value
                else:
                    acc[rows, :] += value
            return carry
        lax.fori_loop(0, R // TM, tile, 0)

    local[0].wait()
    local[1].wait()
    gate_up(s, True)
    gate_up(nb)
    farthest(GU[2:])
    own_x(DN)
    gate_up(xp)
    gate_up(f1)
    gate_up(f2)
    for src in (nb_x, f1_x, f2_x):
        for m, h in GU:
            recv(m, src, h)
        gate_up(src)

    def act(r, carry):
        rows = pl.ds(pl.multiple_of(r * 32, 32), 32)
        g = ga[rows, :]
        hidden[rows, :] = (g / (1.0 + jnp.exp(-g)) * ua[rows, :]).astype(jnp.bfloat16)
        return carry

    lax.fori_loop(0, R // 32, act, 0)

    def down_copy(src, h):
        owner = src // PER
        return owner, pltpu.make_async_remote_copy(
            src_ref=dsend.at[src, h], dst_ref=drecv.at[t, src % PER, h],
            send_sem=d_send.at[src, h], recv_sem=d_recv.at[t, src % PER, h],
            device_id=(s, owner), device_id_type=MESH)

    def down(src, h):
        value = dot(hidden[...], G[2, src, h * HK:(h + 1) * HK, :], NT).astype(jnp.bfloat16)
        owner, c = down_copy(src, h)

        @pl.when(owner != t)
        def _():
            dsend[src, h] = value
            c.start()

        @pl.when(owner == t)
        def _():
            drecv[t, src % PER, h] = value

    local[2].wait()
    near(DN)
    down(s, 0)
    down(s, 1)
    down(nb, 0)
    down(nb, 1)
    middle(DN)
    extra(DN)
    for src in (xp, f1):
        for h in (0, 1):
            down(src, h)
    for h in (1, 0):
        if h == 0:
            farthest(DN)
        recv(2, nb_x, h)
        down(nb_x, h)
    for src in (f2, f1_x, f2_x):
        for h in (0, 1):
            if src is not f2:
                recv(2, src, h)
            down(src, h)

    for i in range(PER):
        for h in (0, 1):
            for peer in reach:
                pltpu.make_async_remote_copy(
                    src_ref=drecv.at[peer, i, h], dst_ref=drecv.at[peer, i, h],
                    send_sem=d_send.at[0, 0], recv_sem=d_recv.at[peer, i, h],
                    device_id=(s, (t + 1) % T), device_id_type=MESH).wait_recv()
            total = drecv[0, i, h].astype(jnp.float32)
            for n in range(1, T):
                total += drecv[n, i, h].astype(jnp.float32)
            cols = slice((i * 2 + h) * HK, (i * 2 + h + 1) * HK)
            out_ref[:, cols] = (after[t, :, cols].astype(jnp.float32) + total).astype(jnp.bfloat16)

    for cond, c in started:
        when(cond, c.wait_send)
    for c in tails + psent + asent:
        c.wait_send()
    for src in range(S):
        for h in (0, 1):
            owner, c = down_copy(src, h)

            @pl.when(owner != t)
            def _():
                c.wait_send()


def fused(residual, queries, keys, values, documents, sinks, out_weight, norm_gain, gate_weight, up_weight, down_weight):
    S, T = lax.axis_size("sp"), lax.axis_size("tp")
    R, D = residual.shape
    F = gate_weight.shape[1]
    C, K = D // T, D // S
    blocks = R // WINDOW
    docs = jnp.broadcast_to(documents.reshape(blocks, 1, WINDOW), (blocks, 8, WINDOW)).reshape(blocks * 8, WINDOW)
    bf, f32 = jnp.bfloat16, jnp.float32
    vm, hbm = pl.BlockSpec(memory_space=pltpu.VMEM), pl.BlockSpec(memory_space=pl.ANY)
    dma = pltpu.SemaphoreType.DMA
    scratch = [
        pltpu.VMEM((3, S, K, F), bf),
        pltpu.VMEM((R + WINDOW, keys.shape[1]), bf),
        pltpu.VMEM((R + WINDOW, keys.shape[1]), bf),
        pltpu.VMEM((blocks * 8 + 8, WINDOW), jnp.int32),
        pltpu.VMEM((R, queries.shape[1]), bf),
        pltpu.VMEM((R, C), bf),
        pltpu.VMEM(out_weight.shape, bf),
        pltpu.VMEM((T, R, C), bf),
        pltpu.VMEM((T, R, C), bf),
        pltpu.VMEM((T, R, C), bf),
        pltpu.VMEM((S, R, K), bf),
        pltpu.VMEM((R, F), f32),
        pltpu.VMEM((R, F), f32),
        pltpu.VMEM((R, F), bf),
        pltpu.VMEM((S, 2, R, K // 2), bf),
        pltpu.VMEM((T, C // K, 2, R, K // 2), bf),
        dma((4, 21)), dma((3, S, 2)), dma((3,)), dma((3,)), dma((5,)),
        dma((T,)), dma((T,)), dma((T,)), dma((T,)), dma((S, 2)), dma((T, C // K, 2)),
    ]
    return pl.pallas_call(
        functools.partial(kernel, S, T),
        out_shape=jax.ShapeDtypeStruct((R, C), bf),
        in_specs=[hbm, vm, vm, vm, vm, pl.BlockSpec(memory_space=pltpu.SMEM), hbm, vm, hbm, hbm, hbm],
        out_specs=vm,
        scratch_shapes=scratch,
        compiler_params=pltpu.CompilerParams(
            collective_id=0, has_side_effects=True, vmem_limit_bytes=60 * 2**20),
    )(residual, queries, keys, values, docs, sinks, out_weight, norm_gain.reshape(1, D),
      gate_weight, up_weight, down_weight)


def line_of_four_pairs(mesh):
    return mesh.shape["sp"] == 8 and mesh.shape["tp"] == 4


def solution(mesh):
    return jax.shard_map(
        fused if line_of_four_pairs(mesh) else on_device,
        mesh=mesh,
        in_specs=(
            P("sp", None),
            P("sp", "tp"),
            P("sp", "tp"),
            P("sp", "tp"),
            P("sp"),
            P("tp"),
            P("tp", None),
            P(),
            P("sp", "tp"),
            P("sp", "tp"),
            P("sp", "tp"),
        ),
        out_specs=P("sp", "tp"),
        check_vma=False,
    )
```
